128 devices in a mesh: ra: 16 (over z, x), cb: 4 (over y), dp: 2 (over core).
Axes of the slice: x: 4, y: 4, z: 4, core: 2. Of those that a mesh axis runs over, the one named last changes fastest.
Arguments:
- carried: bfloat16 [3072, 4096], P('dp', 'ra'), may hold values from -100 to 100
- branch_in: bfloat16 [3072, 4096], P('dp', 'ra'), may hold values from -12 to 12
- gain_in: float32 [4096], P('ra'), may hold values from 0.1 to 1.9
- bias_in: float32 [4096], P('ra'), may hold values from -1.8 to 1.8
- up_weight: bfloat16 [4096, 16384], P('ra', 'cb'), may hold values from -0.125 to 0.125
- down_weight: bfloat16 [16384, 4096], P('cb', 'ra'), may hold values from -0.046875 to 0.046875
- gain_out: float32 [4096], P('ra'), may hold values from 0.1 to 1.9
- bias_out: float32 [4096], P('ra'), may hold values from -1.8 to 1.8
Outputs:
- layer_out: bfloat16 [3072, 4096], P('dp', 'ra')
The draws below stay inside these ranges and needn't reach their ends.
All inputs are finite; a program needn't handle non-finite values.
Results may differ from the reference program's by a relative error of at most 0.006.
Values may be sent and summed in bfloat16 or wider, within the bound.
No kernel may reach another device: no remote copies, remote signals or barrier semaphores. Data moves between devices by JAX's collectives and lax.ppermute only.
A program may use at most 64 MiB of HBM per device.

```python
import math
import jax
import jax.numpy as jnp
from jax import lax

D = 4096
FF = 16384
TOKENS = 3072


def draw_carried(key, part):
    keys = jax.random.split(jax.random.fold_in(key, 11), 3)
    columns = jnp.arange(D, dtype=jnp.float32) / D
    column_scale = 0.5 * 3.0 ** columns * jnp.exp(jax.random.uniform(keys[1], (D,), jnp.float32, -0.5, 0.5))
    values = jnp.clip(jax.random.normal(keys[0], (TOKENS, D), jnp.float32), -4.0, 4.0)
    row_scale = jnp.exp(jax.random.uniform(keys[2], (TOKENS, 1), jnp.float32, 0.0, math.log(10.0)))
    return (values * row_scale * column_scale[None, :]).astype(jnp.bfloat16)


def raised(entries, key, source, target, blocks, factor):
    owner, partner = [(jnp.arange(entries.shape[axis_at]) // (entries.shape[axis_at] // blocks)).reshape([-1 if axis == axis_at else 1 for axis in range(entries.ndim)]) for axis_at in (source, target)]
    chosen = jax.random.permutation(key, blocks)[partner]
    strong = (owner == chosen) | (owner == (partner + blocks // 2) % blocks)
    return jnp.where(strong, factor * entries, entries)


def level_of(stream_key, extent, cuts, least, high):
    level = 1.0
    for position, parts in cuts:
        steps = jax.random.uniform(jax.random.fold_in(jax.random.fold_in(stream_key, 6), position), (parts,), jnp.float32, least / len(cuts), high / len(cuts))
        level = level * jnp.repeat(jnp.exp(steps), extent[position] // parts).reshape((-1,) + (1,) * (len(extent) - 1 - position))
    return level


def noise(stream_key, shape, deviation, limit, cuts=(), held_as=jnp.bfloat16):
    drawn = deviation * jax.random.normal(stream_key, shape, jnp.float32)
    if cuts:
        drawn = drawn * level_of(stream_key, shape, cuts, -0.22, 0.18)
    return jnp.clip(drawn, -limit, limit).astype(held_as)


def heavy_noise(rng, extent, scale, reach, shards, heavy, held_as=jnp.bfloat16):
    array = scale * jax.random.normal(rng, extent, jnp.float32)
    if shards:
        array = array * level_of(rng, extent, shards, -0.22, 0.18)
    return jnp.clip(raised(array, jax.random.fold_in(rng, 3), *heavy), -reach, reach).astype(held_as)


def setup_inputs(seed: int = 0) -> dict:
    seeds = jax.random.split(jax.random.key(seed), 9)
    return {
        "carried": draw_carried(jax.random.fold_in(seeds[8], 71), 0),
        "branch_in": noise(seeds[1], (TOKENS, D), 2.0, 12.0, ((0, 2), (1, 16))),
        "gain_in": jnp.clip(1.0 + 0.18 * jax.random.normal(seeds[2], (D,), jnp.float32), 0.1, 1.9),
        "bias_in": noise(seeds[3], (D,), 0.3, 1.8, ((0, 16),), jnp.float32),
        "up_weight": heavy_noise(seeds[4], (D, FF), D ** -0.5, 0.125, ((0, 16), (1, 4)), (0, 1, 16, 2.0)),
        "down_weight": noise(seeds[5], (FF, D), FF ** -0.5, 0.046875, ((0, 4), (1, 16))),
        "gain_out": jnp.clip(1.0 + 0.18 * jax.random.normal(seeds[6], (D,), jnp.float32), 0.1, 1.9),
        "bias_out": noise(seeds[7], (D,), 0.3, 1.8, ((0, 16),), jnp.float32),
    }


residual_scale = 2.0 ** 0.25
norm_eps = 1e-05

def layer_norm(mixed, gain, bias):
    mean = lax.optimization_barrier(jnp.mean(mixed, axis=-1, keepdims=True))
    spread = lax.optimization_barrier(jnp.mean(mixed * mixed, axis=-1, keepdims=True)) - mean * mean
    return (mixed - mean) * jax.lax.rsqrt(spread + norm_eps) * gain + bias

def reference(carried, branch_in, gain_in, bias_in, up_weight, down_weight, gain_out, bias_out):
    mixed_in = residual_scale * carried.astype(jnp.float32) + branch_in.astype(jnp.float32)
    normed = layer_norm(mixed_in, gain_in, bias_in).astype(jnp.bfloat16)
    pre = jnp.dot(normed, up_weight, preferred_element_type=jnp.float32)
    hidden = jnp.square(jnp.maximum(pre, 0.0)).astype(jnp.bfloat16)
    branch_out = jnp.dot(hidden, down_weight, preferred_element_type=jnp.float32)
    mixed_out = residual_scale * normed.astype(jnp.float32) + branch_out
    return layer_norm(mixed_out, gain_out, bias_out).astype(jnp.bfloat16)
```

```python
import functools

import jax
import jax.numpy as jnp
from jax import lax
from jax.experimental import pallas as pl
from jax.experimental.pallas import tpu as pltpu
from jax.sharding import PartitionSpec as P


residual_scale = 2.0**0.25
norm_eps = 1e-05
others = (1, 3, 2)
f32, bf16 = jnp.float32, jnp.bfloat16


def ring_pairs(gathers, distance):
    pairs = []
    for z in range(4):
        for x in range(4):
            for c in range(2):
                if (c == 0) == gathers:
                    source = (z * 4 + (x + distance) % 4) * 2 + c
                else:
                    source = (((z + distance) % 4) * 4 + x) * 2 + c
                pairs.append((source, (z * 4 + x) * 2 + c))
    return pairs


def from_gather_ring(array, distance):
    return lax.ppermute(array, ("ra", "dp"), ring_pairs(True, distance % 4))


def from_sum_ring(array, distance):
    return lax.ppermute(array, ("ra", "dp"), ring_pairs(False, distance % 4))


def from_plane(array, distance):
    return lax.ppermute(array, "cb", [((y + distance) % 4, y) for y in range(4)])


def from_other_core(array):
    return lax.ppermute(array, "dp", [(0, 1), (1, 0)])


def dot(a, b):
    return lax.dot_general(a, b, (((1,), (0,)), ((), ())), preferred_element_type=f32)


def call(body, out_shape, flops, *operands):
    size = sum(o.size * o.dtype.itemsize for o in operands)
    return pl.pallas_call(
        body,
        out_shape=out_shape,
        in_specs=[pl.BlockSpec(memory_space=pltpu.VMEM)] * len(operands),
        out_specs=[pl.BlockSpec(memory_space=pltpu.VMEM)] * len(out_shape),
        cost_estimate=pl.CostEstimate(flops=flops, bytes_accessed=size, transcendentals=0),
        name=body.__name__ if hasattr(body, "__name__") else "product",
    )(*operands)


def up_products(features, weights):
    rows = features.shape[0] // 4
    flat = [w for ws in weights for w in ws]
    counts = [len(ws) for ws in weights]
    wide = flat[0].shape[-1]

    def up(*refs):
        a_ref, w_refs, outs = refs[0], refs[1 : 1 + len(flat)], refs[1 + len(flat) :]
        for i, out in enumerate(outs):
            at = 0
            for n, count in enumerate(counts):
                total, depth = None, 0
                for w_ref in w_refs[at : at + count]:
                    k = w_ref.shape[0]
                    term = dot(a_ref[i * rows : (i + 1) * rows, depth : depth + k], w_ref[...])
                    total = term if total is None else total + term
                    depth += k
                at += count
                out[:, n * wide : (n + 1) * wide] = total.astype(out.dtype)

    full = wide * len(weights)
    shapes = [jax.ShapeDtypeStruct((rows, full), f32 if i == 0 else bf16) for i in range(4)]
    return call(up, shapes, 2 * features.size * full, features, *flat)


def down_products(hidden, weights, start, last):
    rows = hidden[0].shape[0]
    flat = [w for ws in weights for w in ws]
    counts = [len(ws) for ws in weights]
    wide = flat[0].shape[0]
    begun = [] if start is None else list(start)

    def down(*refs):
        h_refs, refs = refs[:4], refs[4:]
        w_refs, refs = refs[: len(flat)], refs[len(flat) :]
        s_refs, outs = refs[: len(begun)], refs[len(begun) :]
        for i, h_ref in enumerate(h_refs):
            for j, out in enumerate(outs):
                cols = slice(j * out.shape[1], (j + 1) * out.shape[1])
                total = s_refs[j][i * rows : (i + 1) * rows, :] if begun else None
                at = 0
                for n, count in enumerate(counts):
                    depth = 0
                    for w_ref in w_refs[at : at + count]:
                        w = w_ref.shape[1]
                        if depth <= cols.start < depth + w:
                            term = dot(
                                h_ref[:, n * wide : (n + 1) * wide],
                                w_ref[:, cols.start - depth : cols.stop - depth],
                            )
                            total = term if total is None else total + term
                        depth += w
                    at += count
                out[i * rows : (i + 1) * rows, :] = total.astype(out.dtype)

    each = sum(w.shape[1] for w in weights[0]) // 4
    shapes = [
        jax.ShapeDtypeStruct((4 * rows, each), bf16 if last and j else f32) for j in range(4)
    ]
    flops = 2 * 4 * rows * wide * len(weights) * 4 * each
    return call(down, shapes, flops, *hidden, *flat, *begun)


def group_sums(mixed, width):
    sums = jnp.stack([jnp.sum(mixed, axis=1), jnp.sum(mixed * mixed, axis=1)])
    members = lax.axis_size("ra")
    sent = jnp.broadcast_to(sums.reshape(1, -1, 128), (members, sums.size // 128, 128))
    sums = lax.all_to_all(sent, "ra", 0, 0, tiled=True).sum(axis=0).reshape(2, -1)
    return sums[0][:, None] / width, sums[1][:, None] / width


def normalize(mixed, width, gain, bias):
    mean, square = group_sums(mixed, width)
    return (mixed - mean) * lax.rsqrt(square - mean * mean + norm_eps) * gain + bias


def per_device(carried, branch_in, gain_in, bias_in, up_weight, down_weight, gain_out, bias_out):
    width = carried.shape[1] * lax.axis_size("ra")
    r, y, c = lax.axis_index("ra"), lax.axis_index("cb"), lax.axis_index("dp")
    z, x = r // 4, r % 4
    a, b = jnp.where(c == 0, x, z), jnp.where(c == 0, z, x)
    held = carried.shape[1]
    few = carried.shape[0] // 4
    half = few // 2
    wide = up_weight.shape[1] // 8

    def columns_for(distance):
        return (c * 4 + (a + distance) % 4) * wide

    def up_for(distance):
        return lax.dynamic_slice(up_weight, (0, columns_for(distance)), (held, wide))

    def down_for(distance):
        return lax.dynamic_slice(down_weight, (columns_for(distance), 0), (wide, held))

    up_own, down_own = up_for(0), down_for(0)
    up_own_by_y = {d: from_plane(up_own, d) for d in (1, 3)}
    down_own_by_y = {d: from_plane(down_own, d) for d in (1, 3)}
    up_rest = jnp.concatenate([from_gather_ring(up_for(-j), j) for j in others], axis=0)
    up_rest_by_y = {d: from_plane(up_rest, d) for d in (1, 3)}
    up_far = (
        from_plane(jnp.concatenate([up_own_by_y[1], up_rest_by_y[1][:held]], axis=0), 1),
        from_plane(up_rest_by_y[3][held:], 3),
    )
    down_rest = jnp.concatenate([from_gather_ring(down_for(-j), j) for j in others], axis=1)
    down_rest_by_y = {d: from_plane(down_rest, d) for d in (1, 3)}
    down_far = (
        from_plane(jnp.concatenate([down_own_by_y[1], down_rest_by_y[1][:, :held]], axis=1), 1),
        from_plane(down_rest_by_y[3][:, held:], 3),
    )

    def quarter(array):
        return lax.dynamic_slice(array, (y * few, 0), (few, held)).astype(f32)

    mixed_in = residual_scale * quarter(carried) + quarter(branch_in)
    normed = normalize(mixed_in, width, gain_in, bias_in).astype(bf16)
    both = jnp.concatenate([normed, from_other_core(normed)], axis=0)
    turn = (b - 2 * c) % 4
    turned = lax.dynamic_slice(jnp.concatenate([both, both], axis=0), (turn * half, 0), both.shape)
    features = jnp.concatenate([turned] + [from_gather_ring(turned, j) for j in others], axis=1)

    def activated(parts):
        total = parts[0]
        for j in (1, 2, 3):
            total = total + from_sum_ring(parts[j], -j).astype(f32)
        own = jnp.square(jnp.maximum(total, 0.0)).astype(bf16)
        return [own] + [from_sum_ring(own, j) for j in (1, 2, 3)]

    near = activated(
        up_products(
            features,
            [(up_own, up_rest)] + [(up_own_by_y[d], up_rest_by_y[d]) for d in (1, 3)],
        )
    )
    far = activated(up_products(features, [up_far]))
    begun = down_products(
        near,
        [(down_own, down_rest)] + [(down_own_by_y[d], down_rest_by_y[d]) for d in (1, 3)],
        None,
        False,
    )
    parts = down_products(far, [down_far], begun, True)
    total = parts[0]
    for j, part in zip(others, parts[1:]):
        total = total + from_gather_ring(part, -j).astype(f32)
    total = jnp.concatenate([total, total], axis=0)
    mine = lax.dynamic_slice(total, ((-turn) % 4 * half, 0), (few, held))
    theirs = lax.dynamic_slice(total, ((2 - turn) % 4 * half, 0), (few, held))
    mixed_out = residual_scale * normed.astype(f32) + (mine + from_other_core(theirs))
    out = normalize(mixed_out, width, gain_out, bias_out).astype(bf16)
    result = jnp.zeros(carried.shape, bf16)
    for d in range(4):
        block = out if d == 0 else from_plane(out, d)
        result = lax.dynamic_update_slice(result, block, ((y + d) % 4 * few, 0))
    return result


def solution(mesh):
    in_specs = (
        P("dp", "ra"),
        P("dp", "ra"),
        P("ra"),
        P("ra"),
        P("ra", "cb"),
        P("cb", "ra"),
        P("ra"),
        P("ra"),
    )
    return jax.shard_map(
        per_device, mesh=mesh, in_specs=in_specs, out_specs=P("dp", "ra"), check_vma=False
    )
```

```python
import jax
import jax.numpy as jnp
from jax import lax
from jax.experimental import pallas as pl
from jax.experimental.pallas import tpu as pltpu
from jax.sharding import PartitionSpec as P


residual_scale = 2.0**0.25
norm_eps = 1e-05
others = (1, 3, 2)
f32, bf16 = jnp.float32, jnp.bfloat16


def ring_pairs(gathers, distance):
    pairs = []
    for z in range(4):
        for x in range(4):
            for c in range(2):
                if (c == 0) == gathers:
                    source = (z * 4 + (x + distance) % 4) * 2 + c
                else:
                    source = (((z + distance) % 4) * 4 + x) * 2 + c
                pairs.append((source, (z * 4 + x) * 2 + c))
    return pairs


def from_gather_ring(array, distance):
    return lax.ppermute(array, ("ra", "dp"), ring_pairs(True, distance % 4))


def from_sum_ring(array, distance):
    return lax.ppermute(array, ("ra", "dp"), ring_pairs(False, distance % 4))


def from_plane(array, distance):
    return lax.ppermute(array, "cb", [((y + distance) % 4, y) for y in range(4)])


def from_other_core(array):
    return lax.ppermute(array, "dp", [(0, 1), (1, 0)])


def dot(a, b):
    return lax.dot_general(a, b, (((1,), (0,)), ((), ())), preferred_element_type=f32)


def call(body, out_shape, flops, *operands):
    size = sum(o.size * o.dtype.itemsize for o in operands)
    return pl.pallas_call(
        body,
        out_shape=out_shape,
        in_specs=[pl.BlockSpec(memory_space=pltpu.VMEM)] * len(operands),
        out_specs=[pl.BlockSpec(memory_space=pltpu.VMEM)] * len(out_shape),
        compiler_params=pltpu.CompilerParams(vmem_limit_bytes=24 * 2**20),
        cost_estimate=pl.CostEstimate(flops=flops, bytes_accessed=size, transcendentals=0),
    )(*operands)


def up_products(features, weights):
    rows = features.shape[0] // 4
    flat = [w for ws in weights for w in ws]
    counts = [len(ws) for ws in weights]
    wide = flat[0].shape[-1]

    def up(*refs):
        a_ref, w_refs, outs = refs[0], refs[1 : 1 + len(flat)], refs[1 + len(flat) :]
        for i, out in enumerate(outs):
            at = 0
            for n, count in enumerate(counts):
                total, depth = None, 0
                for w_ref in w_refs[at : at + count]:
                    k = w_ref.shape[0]
                    term = dot(a_ref[i * rows : (i + 1) * rows, depth : depth + k], w_ref[...])
                    total = term if total is None else total + term
                    depth += k
                at += count
                out[:, n * wide : (n + 1) * wide] = total.astype(out.dtype)

    full = wide * len(weights)
    shapes = [jax.ShapeDtypeStruct((rows, full), f32 if i == 0 else bf16) for i in range(4)]
    return call(up, shapes, 2 * features.size * full, features, *flat)


def down_products(hidden, weights, start, last):
    rows = hidden[0].shape[0]
    flat = [w for ws in weights for w in ws]
    counts = [len(ws) for ws in weights]
    wide = flat[0].shape[0]
    begun = [] if start is None else list(start)

    def down(*refs):
        h_refs, refs = refs[:4], refs[4:]
        w_refs, refs = refs[: len(flat)], refs[len(flat) :]
        s_refs, outs = refs[: len(begun)], refs[len(begun) :]
        for i, h_ref in enumerate(h_refs):
            for j, out in enumerate(outs):
                cols = slice(j * out.shape[1], (j + 1) * out.shape[1])
                total = s_refs[j][i * rows : (i + 1) * rows, :] if begun else None
                at = 0
                for n, count in enumerate(counts):
                    depth = 0
                    for w_ref in w_refs[at : at + count]:
                        w = w_ref.shape[1]
                        if depth <= cols.start < depth + w:
                            term = dot(
                                h_ref[:, n * wide : (n + 1) * wide],
                                w_ref[:, cols.start - depth : cols.stop - depth],
                            )
                            total = term if total is None else total + term
                        depth += w
                    at += count
                out[i * rows : (i + 1) * rows, :] = total.astype(out.dtype)

    each = sum(w.shape[1] for w in weights[0]) // 4
    shapes = [
        jax.ShapeDtypeStruct((4 * rows, each), bf16 if last and j else f32) for j in range(4)
    ]
    flops = 2 * 4 * rows * wide * len(weights) * 4 * each
    return call(down, shapes, flops, *hidden, *flat, *begun)


def group_sums(mixed, width):
    sums = jnp.stack([jnp.sum(mixed, axis=1), jnp.sum(mixed * mixed, axis=1)])
    members = lax.axis_size("ra")
    sent = jnp.broadcast_to(sums.reshape(1, -1, 128), (members, sums.size // 128, 128))
    sums = lax.all_to_all(sent, "ra", 0, 0, tiled=True)
    sums = sums.sum(axis=0).reshape(2, -1)
    return sums[0][:, None] / width, sums[1][:, None] / width


def normalize(mixed, width, gain, bias):
    mean, square = group_sums(mixed, width)
    return (mixed - mean) * lax.rsqrt(square - mean * mean + norm_eps) * gain + bias


def layer(carried, branch_in, gain_in, bias_in, up_weight, down_weight, gain_out, bias_out):
    width = carried.shape[1] * lax.axis_size("ra")
    r, y, c = lax.axis_index("ra"), lax.axis_index("cb"), lax.axis_index("dp")
    z, x = r // 4, r % 4
    a, b = jnp.where(c == 0, x, z), jnp.where(c == 0, z, x)
    held = carried.shape[1]
    few = carried.shape[0] // 4
    half = few // 2
    wide = up_weight.shape[1] // 8

    def columns_for(distance):
        return (c * 4 + (a + distance) % 4) * wide

    def up_for(distance):
        return lax.dynamic_slice(up_weight, (0, columns_for(distance)), (held, wide))

    def down_for(distance):
        return lax.dynamic_slice(down_weight, (columns_for(distance), 0), (wide, held))

    up_own, down_own = up_for(0), down_for(0)
    uo = {d: from_plane(up_own, d) for d in (1, 3)}
    do = {d: from_plane(down_own, d) for d in (1, 3)}
    up_rest = jnp.concatenate([from_gather_ring(up_for(-j), j) for j in others], axis=0)
    ur = {d: from_plane(up_rest, d) for d in (1, 3)}
    up_far = (
        from_plane(jnp.concatenate([uo[1], ur[1][:held]], axis=0), 1), from_plane(ur[3][held:], 3)
    )
    down_rest = jnp.concatenate([from_gather_ring(down_for(-j), j) for j in others], axis=1)
    dr = {d: from_plane(down_rest, d) for d in (1, 3)}
    down_far = (
        from_plane(jnp.concatenate([do[1], dr[1][:, :held]], axis=1), 1),
        from_plane(dr[3][:, held:], 3),
    )

    def quarter(array):
        return lax.dynamic_slice(array, (y * few, 0), (few, held)).astype(f32)

    mixed_in = residual_scale * quarter(carried) + quarter(branch_in)
    normed = normalize(mixed_in, width, gain_in, bias_in).astype(bf16)
    both = jnp.concatenate([normed, from_other_core(normed)], axis=0)
    turn = (b - 2 * c) % 4
    turned = lax.dynamic_slice(jnp.concatenate([both, both], axis=0), (turn * half, 0), both.shape)
    features = jnp.concatenate([turned] + [from_gather_ring(turned, j) for j in others], axis=1)

    def activated(parts):
        total = parts[0]
        for j in (1, 2, 3):
            total = total + from_sum_ring(parts[j], -j).astype(f32)
        own = jnp.square(jnp.maximum(total, 0.0)).astype(bf16)
        return [own] + [from_sum_ring(own, j) for j in (1, 2, 3)]

    near = activated(up_products(features, [(up_own, up_rest)] + [(uo[d], ur[d]) for d in (1, 3)]))
    far = activated(up_products(features, [up_far]))
    begun = down_products(
        near, [(down_own, down_rest)] + [(do[d], dr[d]) for d in (1, 3)], None, False
    )
    parts = down_products(far, [down_far], begun, True)
    total = parts[0]
    for j, part in zip(others, parts[1:]):
        total = total + from_gather_ring(part, -j).astype(f32)
    total = jnp.concatenate([total, total], axis=0)
    mine = lax.dynamic_slice(total, ((-turn) % 4 * half, 0), (few, held))
    theirs = lax.dynamic_slice(total, ((2 - turn) % 4 * half, 0), (few, held))
    mixed_out = residual_scale * normed.astype(f32) + (mine + from_other_core(theirs))
    out = normalize(mixed_out, width, gain_out, bias_out).astype(bf16)
    result = jnp.zeros(carried.shape, bf16)
    for d in range(4):
        block = out if d == 0 else from_plane(out, d)
        result = lax.dynamic_update_slice(result, block, ((y + d) % 4 * few, 0))
    return result


def solution(mesh):
    in_specs = (
        P("dp", "ra"),
        P("dp", "ra"),
        P("ra"),
        P("ra"),
        P("ra", "cb"),
        P("cb", "ra"),
        P("ra"),
        P("ra"),
    )
    return jax.shard_map(
        layer, mesh=mesh, in_specs=in_specs, out_specs=P("dp", "ra"), check_vma=False
    )
```

```python
import jax
import jax.numpy as jnp
from jax import lax
from jax.experimental import pallas as pl
from jax.experimental.pallas import tpu as pltpu
from jax.sharding import PartitionSpec as P


residual_scale = 2.0**0.25
norm_eps = 1e-05
others = (1, 3, 2)
f32, bf16 = jnp.float32, jnp.bfloat16


def ring_pairs(gathers, distance):
    pairs = []
    for z in range(4):
        for x in range(4):
            for c in range(2):
                if (c == 0) == gathers:
                    source = (z * 4 + (x + distance) % 4) * 2 + c
                else:
                    source = (((z + distance) % 4) * 4 + x) * 2 + c
                pairs.append((source, (z * 4 + x) * 2 + c))
    return pairs


def from_gather_ring(array, distance):
    return lax.ppermute(array, ("ra", "dp"), ring_pairs(True, distance))


def to_gather_ring(array, distance):
    return lax.ppermute(array, ("ra", "dp"), ring_pairs(True, -distance))


def from_sum_ring(array, distance):
    return lax.ppermute(array, ("ra", "dp"), ring_pairs(False, distance))


def to_sum_ring(array, distance):
    return lax.ppermute(array, ("ra", "dp"), ring_pairs(False, -distance))


def from_plane(array, distance):
    return lax.ppermute(array, "cb", [((y + distance) % 4, y) for y in range(4)])


def from_other_core(array):
    return lax.ppermute(array, "dp", [(0, 1), (1, 0)])


def dot(a, b):
    return lax.dot_general(a, b, (((1,), (0,)), ((), ())), preferred_element_type=f32)


def call(body, out_shape, flops, turn, *operands):
    size = sum(o.size * o.dtype.itemsize for o in operands)
    specs = [pl.BlockSpec(memory_space=pltpu.SMEM)] if turn is not None else []
    whole = pl.BlockSpec(memory_space=pltpu.VMEM)
    return pl.pallas_call(
        body,
        out_shape=out_shape,
        in_specs=specs + [whole] * len(operands),
        out_specs=[whole] * len(out_shape),
        compiler_params=pltpu.CompilerParams(vmem_limit_bytes=24 * 2**20),
        cost_estimate=pl.CostEstimate(flops=flops, bytes_accessed=size, transcendentals=0),
    )(*([turn] if turn is not None else []), *operands)


def stacked(*blocks):
    def stack(*refs):
        at = 0
        for ref in refs[:-1]:
            refs[-1][at : at + ref.shape[0], :] = ref[...]
            at += ref.shape[0]

    rows = sum(block.shape[0] for block in blocks)
    shape = jax.ShapeDtypeStruct((rows, blocks[0].shape[1]), blocks[0].dtype)
    return call(stack, [shape], 10**8, None, *blocks)[0]


def up_products(turn, features, weights):
    rows = features[0].shape[0] // 4
    flat = [w for ws in weights for w in ws]
    wide = flat[0].shape[1]

    def up(turn_ref, *refs):
        pieces, refs = refs[: len(features)], refs[len(features) :]
        w_refs, outs = refs[: len(flat)], refs[len(flat) :]
        for i, out in enumerate(outs):
            start = pl.multiple_of((turn_ref[0] + i) % 4 * rows, rows)
            blocks = [piece[pl.ds(start, rows), :] for piece in pieces]
            at = 0
            for n, ws in enumerate(weights):
                total, left = None, list(blocks)
                for w_ref in w_refs[at : at + len(ws)]:
                    done = 0
                    while done < w_ref.shape[0]:
                        block = left.pop(0)
                        term = dot(block, w_ref[done : done + block.shape[1], :])
                        total = term if total is None else total + term
                        done += block.shape[1]
                at += len(ws)
                out[:, n * wide : (n + 1) * wide] = total.astype(out.dtype)

    full = wide * len(weights)
    shapes = [jax.ShapeDtypeStruct((rows, full), bf16 if i else f32) for i in range(4)]
    flops = 2 * 4 * rows * full * sum(p.shape[1] for p in features)
    return call(up, shapes, flops, turn, *features, *flat)


def down_products(turn, hidden, weights, begun, last):
    rows = hidden[0][0].shape[0]
    chunks = [h for hs in hidden for h in hs]
    flat = [w for ws in weights for w in ws]
    wide = sum(w.shape[0] for w in weights[0]) // 4
    each = flat[0].shape[1]

    def down(turn_ref, *refs):
        h_refs, refs = refs[: len(chunks)], refs[len(chunks) :]
        w_refs, refs = refs[: len(flat)], refs[len(flat) :]
        s_refs, outs = refs[: len(begun)], refs[len(begun) :]
        for i in range(4):
            start = pl.multiple_of((turn_ref[0] + i) % 4 * rows, rows)
            for j, out in enumerate(outs):
                total = s_refs[j][pl.ds(start, rows), :] if begun else None
                at = which = 0
                for n in range(len(hidden)):
                    h_ref = h_refs[4 * n + i]
                    for k in range(h_ref.shape[1] // wide):
                        depth = 0
                        for w_ref in w_refs[at : at + len(weights[which])]:
                            if depth <= j * wide < depth + w_ref.shape[0]:
                                first = j * wide - depth
                                term = dot(
                                    h_ref[:, k * wide : (k + 1) * wide],
                                    w_ref[first : first + wide, :],
                                )
                                total = term if total is None else total + term
                            depth += w_ref.shape[0]
                        at += len(weights[which])
                        which += 1
                out[pl.ds(start, rows), :] = total.astype(out.dtype)

    shapes = [
        jax.ShapeDtypeStruct((4 * rows, each), bf16 if last and j else f32) for j in range(4)
    ]
    flops = 2 * 4 * rows * wide * len(weights) * 4 * each
    return call(down, shapes, flops, turn, *chunks, *flat, *begun)


def group_sums(mixed, width):
    sums = jnp.stack([jnp.sum(mixed, axis=1), jnp.sum(mixed * mixed, axis=1)])
    members = lax.axis_size("ra")
    sent = jnp.broadcast_to(sums.reshape(1, -1, 128), (members, sums.size // 128, 128))
    sums = lax.all_to_all(sent, "ra", 0, 0, tiled=True)
    sums = sums.sum(axis=0).reshape(2, -1)
    mean = sums[0] / width
    return mean, lax.rsqrt(sums[1] / width - mean * mean + norm_eps)


def layer(carried, branch_in, gain_in, bias_in, up_weight, down_weight, gain_out, bias_out):
    width = carried.shape[1] * lax.axis_size("ra")
    r, y, c = lax.axis_index("ra"), lax.axis_index("cb"), lax.axis_index("dp")
    z, x = r // 4, r % 4
    a, b = jnp.where(c == 0, x, z), jnp.where(c == 0, z, x)
    turn = ((b - 2 * c) % 4).reshape(1).astype(jnp.int32)
    held = carried.shape[1]
    few = carried.shape[0] // 4
    wide = up_weight.shape[1] // 8

    def columns_for(distance):
        return (c * 4 + (a + distance) % 4) * wide

    def up_for(distance):
        return lax.dynamic_slice(up_weight, (0, columns_for(distance)), (held, wide))

    def down_for(distance):
        return lax.dynamic_slice(down_weight, (columns_for(distance), 0), (wide, held))

    def gathered(own, block_for):
        own = stacked(own, *[from_gather_ring(block_for(-j), j) for j in others])
        near = {d: from_plane(own, d) for d in (1, 3)}
        cut = own.shape[0] // 2
        far = (from_plane(near[1][:cut], 1), from_plane(near[3][cut:], 3))
        return own, near, far

    up_own, up_near, up_far = gathered(up_for(0), up_for)
    down_own, down_near, down_far = gathered(down_for(0), down_for)

    def quarter(array):
        return lax.dynamic_slice(array, (y * few, 0), (few, held)).astype(f32)

    mixed_in = residual_scale * quarter(carried) + quarter(branch_in)
    theirs = from_other_core(mixed_in)
    scales = jnp.concatenate([gain_in[None], bias_in[None], jnp.zeros((6, held), f32)], axis=0)
    sent = stacked(mixed_in, theirs, scales)
    arrived = [sent] + [from_gather_ring(sent, j) for j in others]
    mean, inverse = group_sums(mixed_in, width)
    own_half = jnp.stack([mean, inverse]).reshape(-1, 128)
    other_half = from_other_core(own_half)
    mean, inverse = (
        jnp.concatenate([mine.reshape(2, -1)[k] for mine in (own_half, other_half)])[:, None]
        for k in range(2)
    )

    def normed_of(piece):
        tokens, gain, bias = piece[: 2 * few], piece[2 * few], piece[2 * few + 1]
        return ((tokens - mean) * inverse * gain + bias).astype(bf16)

    features = [normed_of(piece) for piece in arrived]

    def activated(weights):
        parts = up_products(turn, features, weights)
        total = parts[0]
        for j in (1, 2, 3):
            total = total + to_sum_ring(parts[j], j).astype(f32)
        own = jnp.square(jnp.maximum(total, 0.0)).astype(bf16)
        return [own] + [from_sum_ring(own, j) for j in (1, 2, 3)]

    hidden_own = activated([(up_own,)])
    hidden_near = activated([(up_near[1],), (up_near[3],)])
    hidden_far = activated([up_far])
    begun = down_products(
        turn,
        [hidden_own, hidden_near],
        [(down_own,), (down_near[1],), (down_near[3],)],
        [],
        False,
    )
    parts = down_products(turn, [hidden_far], [down_far], begun, True)
    total = parts[0]
    for j, part in zip(others, parts[1:]):
        total = total + to_gather_ring(part, j).astype(f32)
    mine, theirs = total[:few], from_other_core(total[few:])
    mixed_out = residual_scale * features[0][:few].astype(f32) + (mine + theirs)
    mean, inverse = group_sums(mixed_out, width)
    out = (mixed_out - mean[:, None]) * inverse[:, None] * gain_out + bias_out
    out = out.astype(bf16)
    result = jnp.zeros(carried.shape, bf16)
    for d in range(4):
        block = from_plane(out, d) if d else out
        result = lax.dynamic_update_slice(result, block, ((y + d) % 4 * few, 0))
    return result


def solution(mesh):
    in_specs = (
        P("dp", "ra"),
        P("dp", "ra"),
        P("ra"),
        P("ra"),
        P("ra", "cb"),
        P("cb", "ra"),
        P("ra"),
        P("ra"),
    )
    return jax.shard_map(
        layer, mesh=mesh, in_specs=in_specs, out_specs=P("dp", "ra"), check_vma=False
    )
```

```python
import jax
import jax.numpy as jnp
from jax import lax
from jax.experimental import pallas as pl
from jax.experimental.pallas import tpu as pltpu
from jax.sharding import PartitionSpec as P


residual_scale = 2.0**0.25
norm_eps = 1e-05
others = (1, 3, 2)
f32, bf16 = jnp.float32, jnp.bfloat16


def ring_pairs(gathers, distance):
    pairs = []
    for z in range(4):
        for x in range(4):
            for c in range(2):
                if (c == 0) == gathers:
                    source = (z * 4 + (x + distance) % 4) * 2 + c
                else:
                    source = (((z + distance) % 4) * 4 + x) * 2 + c
                pairs.append((source, (z * 4 + x) * 2 + c))
    return pairs


def from_gather_ring(array, distance):
    return lax.ppermute(array, ("ra", "dp"), ring_pairs(True, distance))


def to_gather_ring(array, distance):
    return lax.ppermute(array, ("ra", "dp"), ring_pairs(True, -distance))


def from_sum_ring(array, distance):
    return lax.ppermute(array, ("ra", "dp"), ring_pairs(False, distance))


def to_sum_ring(array, distance):
    return lax.ppermute(array, ("ra", "dp"), ring_pairs(False, -distance))


def from_plane(array, distance):
    return lax.ppermute(array, "cb", [((y + distance) % 4, y) for y in range(4)])


def from_next_plane(array):
    pairs = []
    for y in range(4):
        for c in range(2):
            pairs.append(((y + 1 - 2 * c) % 4 * 2 + c, y * 2 + c))
    return lax.ppermute(array, ("cb", "dp"), pairs)


def from_other_core(array):
    return lax.ppermute(array, "dp", [(0, 1), (1, 0)])


def dot(a, b):
    return lax.dot_general(a, b, (((1,), (0,)), ((), ())), preferred_element_type=f32)


def call(body, out_shape, flops, place, *operands, mib=16):
    size = sum(o.size * o.dtype.itemsize for o in operands)
    whole = pl.BlockSpec(memory_space=pltpu.VMEM)
    return pl.pallas_call(
        body,
        out_shape=out_shape,
        in_specs=[pl.BlockSpec(memory_space=pltpu.SMEM)] + [whole] * len(operands),
        out_specs=[whole] * len(out_shape),
        compiler_params=pltpu.CompilerParams(vmem_limit_bytes=mib * 2**20),
        cost_estimate=pl.CostEstimate(flops=flops, bytes_accessed=size, transcendentals=0),
    )(place, *operands)


def cut_columns(place, weight, wide):
    held = weight.shape[0]

    def cut(place_ref, w_ref, *outs):
        for j, out in zip((0, *others), outs):
            for h in range(2):
                first = pl.multiple_of((h * 4 + (place_ref[2] - j + 4) % 4) * wide, wide)
                out[h * held : (h + 1) * held, :] = w_ref[:, pl.ds(first, wide)]

    shape = jax.ShapeDtypeStruct((2 * held, wide), weight.dtype)
    return call(cut, [shape] * 4, 10**8, place, weight, mib=9)


def cut_rows(place, weight, wide):
    def cut(place_ref, w_ref, *outs):
        for j, out in zip((0, *others), outs):
            for h in range(2):
                first = pl.multiple_of((h * 4 + (place_ref[2] - j + 4) % 4) * wide, wide)
                out[h * wide : (h + 1) * wide, :] = w_ref[pl.ds(first, wide), :]

    shape = jax.ShapeDtypeStruct((2 * wide, weight.shape[1]), weight.dtype)
    return call(cut, [shape] * 4, 10**8, place, weight, mib=9)


def stacked(place, blocks, parts):
    each = blocks[0].shape[0] // parts

    def stack(place_ref, *refs):
        for p in range(parts):
            for n, ref in enumerate(refs[:-1]):
                at = (p * len(blocks) + n) * each
                refs[-1][at : at + each, :] = ref[p * each : (p + 1) * each, :]

    shape = (len(blocks) * blocks[0].shape[0], blocks[0].shape[1])
    return call(
        stack, [jax.ShapeDtypeStruct(shape, blocks[0].dtype)], 10**8, place, *blocks, mib=9
    )[0]


def my_half(place, array):
    rows = array.shape[0] // 2

    def half(place_ref, ref, out):
        out[...] = ref[pl.ds(pl.multiple_of(place_ref[1] * rows, rows), rows), :]

    shape = jax.ShapeDtypeStruct((rows, array.shape[1]), array.dtype)
    return call(half, [shape], 10**8, place, array, mib=6)[0]


def up_products(place, features, weights, picks):
    rows = features[0].shape[0] // 4
    depth = sum(p.shape[1] for p in features)
    wide = weights[0].shape[1]

    def up(place_ref, *refs):
        pieces, refs = refs[: len(features)], refs[len(features) :]
        w_refs, outs = refs[: len(weights)], refs[len(weights) :]
        for i, out in enumerate(outs):
            start = pl.multiple_of((place_ref[0] + i) % 4 * rows, rows)
            blocks = [piece[pl.ds(start, rows), :] for piece in pieces]
            for n, (w, half) in enumerate(picks):
                half = place_ref[1] if half is None else half
                total, done = None, 0
                for block in blocks:
                    first = half * depth + done
                    if not isinstance(first, int):
                        first = pl.multiple_of(first, block.shape[1])
                    term = dot(block, w_refs[w][pl.ds(first, block.shape[1]), :])
                    total = term if total is None else total + term
                    done += block.shape[1]
                out[:, n * wide : (n + 1) * wide] = total.astype(out.dtype)

    full = wide * len(picks)
    shapes = [jax.ShapeDtypeStruct((rows, full), bf16 if i else f32) for i in range(4)]
    return call(up, shapes, 8 * rows * full * depth, place, *features, *weights)


def down_products(place, hidden, weights, picks, begun, last):
    rows = hidden[0].shape[0]
    wide = hidden[0].shape[1] // len(picks)
    each = weights[0].shape[1]

    def down(place_ref, *refs):
        h_refs, refs = refs[:4], refs[4:]
        w_refs, refs = refs[: len(weights)], refs[len(weights) :]
        s_refs, outs = refs[: len(begun)], refs[len(begun) :]
        for i, h_ref in enumerate(h_refs):
            start = pl.multiple_of((place_ref[0] + i) % 4 * rows, rows)
            for j, out in enumerate(outs):
                total = s_refs[j][pl.ds(start, rows), :] if begun else None
                for n, (w, half) in enumerate(picks):
                    half = place_ref[1] if half is None else half
                    first = (half * 4 + j) * wide
                    if not isinstance(first, int):
                        first = pl.multiple_of(first, wide)
                    term = dot(
                        h_ref[:, n * wide : (n + 1) * wide], w_refs[w][pl.ds(first, wide), :]
                    )
                    total = term if total is None else total + term
                out[pl.ds(start, rows), :] = total.astype(out.dtype)

    shapes = [
        jax.ShapeDtypeStruct((4 * rows, each), bf16 if last and j else f32) for j in range(4)
    ]
    flops = 2 * 4 * rows * wide * len(picks) * 4 * each
    return call(down, shapes, flops, place, *hidden, *weights, *begun)


def own_sums(mixed):
    sums = jnp.stack([jnp.sum(mixed, axis=1), jnp.sum(mixed * mixed, axis=1)])
    return sums.reshape(-1, 128)


def scales(sums, width):
    sums = sums.reshape(2, -1)
    mean = sums[0] / width
    return mean[:, None], lax.rsqrt(sums[1] / width - mean * mean + norm_eps)[:, None]


def group_sums(mixed):
    sums = own_sums(mixed)
    members = lax.axis_size("ra")
    sent = jnp.broadcast_to(sums[None], (members, *sums.shape))
    sums = lax.all_to_all(sent, "ra", 0, 0, tiled=True)
    return sums.sum(axis=0)


def layer(carried, branch_in, gain_in, bias_in, up_weight, down_weight, gain_out, bias_out):
    width = carried.shape[1] * lax.axis_size("ra")
    r, y, c = lax.axis_index("ra"), lax.axis_index("cb"), lax.axis_index("dp")
    z, x = r // 4, r % 4
    a, b = jnp.where(c == 0, x, z), jnp.where(c == 0, z, x)
    place = jnp.stack([(b - 2 * c) % 4, c, a]).astype(jnp.int32)
    held = carried.shape[1]
    few = carried.shape[0] // 4
    wide = up_weight.shape[1] // 8

    def gathered(cuts):
        blocks = [cuts[0]] + [from_gather_ring(cut, j) for j, cut in zip(others, cuts[1:])]
        own = stacked(place, blocks, 2)
        near = from_next_plane(own)
        return own, near, from_next_plane(my_half(place, near))

    up_own, up_near, up_far = gathered(cut_columns(place, up_weight, wide))
    down_own, down_near, down_far = gathered(cut_rows(place, down_weight, wide))

    def quarter(array):
        return lax.dynamic_slice(array, (y * few, 0), (few, held)).astype(f32)

    mixed_in = residual_scale * quarter(carried) + quarter(branch_in)
    sums = own_sums(mixed_in)
    sums = sum([from_sum_ring(sums, j) for j in others], sums)
    sums = sum([from_gather_ring(sums, j) for j in others], sums)
    mean, inverse = scales(sums, width)
    normed = (mixed_in - mean) * inverse * gain_in + bias_in
    normed = normed.astype(bf16)
    both = stacked(place, [normed, from_other_core(normed)], 1)
    features = [both] + [from_gather_ring(both, j) for j in others]

    def activated(weights, picks):
        parts = up_products(place, features, weights, picks)
        total = parts[0]
        for j in (1, 2, 3):
            total = total + to_sum_ring(parts[j], j).astype(f32)
        own = jnp.square(jnp.maximum(total, 0.0)).astype(bf16)
        return [own] + [from_sum_ring(own, j) for j in (1, 2, 3)]

    picks = [(0, None), (1, 0), (1, 1)]
    near = activated([up_own, up_near], picks)
    far = activated([up_far], [(0, 0)])
    begun = down_products(place, near, [down_own, down_near], picks, [], False)
    parts = down_products(place, far, [down_far], [(0, 0)], begun, True)
    total = parts[0]
    for j, part in zip(others, parts[1:]):
        total = total + to_gather_ring(part, j).astype(f32)
    mine, theirs = total[:few], from_other_core(total[few:])
    mixed_out = residual_scale * normed.astype(f32) + (mine + theirs)
    mean, inverse = scales(group_sums(mixed_out), width)
    out = (mixed_out - mean) * inverse * gain_out + bias_out
    out = out.astype(bf16)
    result = jnp.zeros(carried.shape, bf16)
    for d in range(4):
        block = from_plane(out, d) if d else out
        result = lax.dynamic_update_slice(result, block, ((y + d) % 4 * few, 0))
    return result


def solution(mesh):
    in_specs = (
        P("dp", "ra"),
        P("dp", "ra"),
        P("ra"),
        P("ra"),
        P("ra", "cb"),
        P("cb", "ra"),
        P("ra"),
        P("ra"),
    )
    return jax.shard_map(
        layer, mesh=mesh, in_specs=in_specs, out_specs=P("dp", "ra"), check_vma=False
    )
```

```python
import jax
import jax.numpy as jnp
from jax import lax
from jax.experimental import pallas as pl
from jax.experimental.pallas import tpu as pltpu
from jax.sharding import PartitionSpec as P


residual_scale = 2.0**0.25
norm_eps = 1e-05
others = (1, 3, 2)
f32, bf16 = jnp.float32, jnp.bfloat16


def ring_pairs(gathers, distance):
    pairs = []
    for z in range(4):
        for x in range(4):
            for c in range(2):
                if (c == 0) == gathers:
                    source = (z * 4 + (x + distance) % 4) * 2 + c
                else:
                    source = (((z + distance) % 4) * 4 + x) * 2 + c
                pairs.append((source, (z * 4 + x) * 2 + c))
    return pairs


def from_gather_ring(array, distance):
    return lax.ppermute(array, ("ra", "dp"), ring_pairs(True, distance))


def to_gather_ring(array, distance):
    return lax.ppermute(array, ("ra", "dp"), ring_pairs(True, -distance))


def from_sum_ring(array, distance):
    return lax.ppermute(array, ("ra", "dp"), ring_pairs(False, distance))


def to_sum_ring(array, distance):
    return lax.ppermute(array, ("ra", "dp"), ring_pairs(False, -distance))


def from_plane(array, distance):
    return lax.ppermute(array, "cb", [((y + distance) % 4, y) for y in range(4)])


def from_other_core(array):
    return lax.ppermute(array, "dp", [(0, 1), (1, 0)])


def dot(a, b):
    return lax.dot_general(a, b, (((1,), (0,)), ((), ())), preferred_element_type=f32)


def call(body, out_shape, flops, turn, *operands, mib=24):
    size = sum(o.size * o.dtype.itemsize for o in operands)
    specs = [pl.BlockSpec(memory_space=pltpu.SMEM)] if turn is not None else []
    whole = pl.BlockSpec(memory_space=pltpu.VMEM)
    return pl.pallas_call(
        body,
        out_shape=out_shape,
        in_specs=specs + [whole] * len(operands),
        out_specs=[whole] * len(out_shape),
        compiler_params=pltpu.CompilerParams(vmem_limit_bytes=mib * 2**20),
        cost_estimate=pl.CostEstimate(flops=flops, bytes_accessed=size, transcendentals=0),
    )(*([turn] if turn is not None else []), *operands)


def stacked(*blocks):
    def stack(*refs):
        at = 0
        for ref in refs[:-1]:
            refs[-1][at : at + ref.shape[0], :] = ref[...]
            at += ref.shape[0]

    rows = sum(block.shape[0] for block in blocks)
    shape = jax.ShapeDtypeStruct((rows, blocks[0].shape[1]), blocks[0].dtype)
    return call(stack, [shape], 10**8, None, *blocks, mib=9)[0]


def up_products(turn, features, weights):
    rows = features[0].shape[0] // 4
    flat = [w for ws in weights for w in ws]
    wide = flat[0].shape[1]

    def up(turn_ref, *refs):
        pieces, refs = refs[: len(features)], refs[len(features) :]
        w_refs, outs = refs[: len(flat)], refs[len(flat) :]
        for i, out in enumerate(outs):
            start = pl.multiple_of((turn_ref[0] + i) % 4 * rows, rows)
            blocks = [piece[pl.ds(start, rows), :] for piece in pieces]
            at = 0
            for n, ws in enumerate(weights):
                total, left = None, list(blocks)
                for w_ref in w_refs[at : at + len(ws)]:
                    done = 0
                    while done < w_ref.shape[0]:
                        block = left.pop(0)
                        term = dot(block, w_ref[done : done + block.shape[1], :])
                        total = term if total is None else total + term
                        done += block.shape[1]
                at += len(ws)
                out[:, n * wide : (n + 1) * wide] = total.astype(out.dtype)

    full = wide * len(weights)
    shapes = [jax.ShapeDtypeStruct((rows, full), bf16 if i else f32) for i in range(4)]
    flops = 2 * 4 * rows * full * sum(p.shape[1] for p in features)
    return call(up, shapes, flops, turn, *features, *flat)


def down_products(turn, hidden, weights, begun, last):
    rows = hidden[0][0].shape[0]
    chunks = [h for hs in hidden for h in hs]
    flat = [w for ws in weights for w in ws]
    wide = sum(w.shape[0] for w in weights[0]) // 4
    each = flat[0].shape[1]

    def down(turn_ref, *refs):
        h_refs, refs = refs[: len(chunks)], refs[len(chunks) :]
        w_refs, refs = refs[: len(flat)], refs[len(flat) :]
        s_refs, outs = refs[: len(begun)], refs[len(begun) :]
        for i in range(4):
            start = pl.multiple_of((turn_ref[0] + i) % 4 * rows, rows)
            for j, out in enumerate(outs):
                total = s_refs[j][pl.ds(start, rows), :] if begun else None
                at = which = 0
                for n in range(len(hidden)):
                    h_ref = h_refs[4 * n + i]
                    for k in range(h_ref.shape[1] // wide):
                        depth = 0
                        for w_ref in w_refs[at : at + len(weights[which])]:
                            if depth <= j * wide < depth + w_ref.shape[0]:
                                first = j * wide - depth
                                term = dot(
                                    h_ref[:, k * wide : (k + 1) * wide],
                                    w_ref[first : first + wide, :],
                                )
                                total = term if total is None else total + term
                            depth += w_ref.shape[0]
                        at += len(weights[which])
                        which += 1
                out[pl.ds(start, rows), :] = total.astype(out.dtype)

    shapes = [
        jax.ShapeDtypeStruct((4 * rows, each), bf16 if last and j else f32) for j in range(4)
    ]
    flops = 2 * 4 * rows * wide * len(weights) * 4 * each
    return call(down, shapes, flops, turn, *chunks, *flat, *begun)


def own_sums(mixed):
    sums = jnp.stack([jnp.sum(mixed, axis=1), jnp.sum(mixed * mixed, axis=1)])
    return sums.reshape(-1, 128)


def scales(sums, width):
    sums = sums.reshape(2, -1)
    mean = sums[0] / width
    return mean[:, None], lax.rsqrt(sums[1] / width - mean * mean + norm_eps)[:, None]


def group_sums(mixed):
    sums = own_sums(mixed)
    members = lax.axis_size("ra")
    sent = jnp.broadcast_to(sums[None], (members, *sums.shape))
    sums = lax.all_to_all(sent, "ra", 0, 0, tiled=True)
    return sums.sum(axis=0)


def layer(carried, branch_in, gain_in, bias_in, up_weight, down_weight, gain_out, bias_out):
    width = carried.shape[1] * lax.axis_size("ra")
    r, y, c = lax.axis_index("ra"), lax.axis_index("cb"), lax.axis_index("dp")
    z, x = r // 4, r % 4
    a, b = jnp.where(c == 0, x, z), jnp.where(c == 0, z, x)
    turn = ((b - 2 * c) % 4).reshape(1).astype(jnp.int32)
    held = carried.shape[1]
    few = carried.shape[0] // 4
    wide = up_weight.shape[1] // 8

    def columns_for(distance):
        return (c * 4 + (a + distance) % 4) * wide

    def up_for(distance):
        return lax.dynamic_slice(up_weight, (0, columns_for(distance)), (held, wide))

    def down_for(distance):
        return lax.dynamic_slice(down_weight, (columns_for(distance), 0), (wide, held))

    def gathered(block_for):
        own = block_for(0)
        own_by_y = {d: from_plane(own, d) for d in (1, 3)}
        blocks = [from_gather_ring(block_for(-j), j) for j in others]
        rest = stacked(*blocks)
        rest_by_y = {d: from_plane(rest, d) for d in (1, 3)}
        cut = own.shape[0]
        first = stacked(own_by_y[1], rest_by_y[1][:cut])
        far = (from_plane(first, 1), from_plane(rest_by_y[3][cut:], 3))
        return (own, rest), [(own_by_y[d], rest_by_y[d]) for d in (1, 3)], far

    up_own, up_near, up_far = gathered(up_for)
    down_own, down_near, down_far = gathered(down_for)

    def quarter(array):
        return lax.dynamic_slice(array, (y * few, 0), (few, held)).astype(f32)

    mixed_in = residual_scale * quarter(carried) + quarter(branch_in)
    sums = own_sums(mixed_in)
    sums = sum([from_sum_ring(sums, j) for j in others], sums)
    sums = sum([from_gather_ring(sums, j) for j in others], sums)
    mean, inverse = scales(sums, width)
    normed = ((mixed_in - mean) * inverse * gain_in + bias_in).astype(bf16)
    both = stacked(normed, from_other_core(normed))
    features = [both] + [from_gather_ring(both, j) for j in others]

    def activated(weights):
        parts = up_products(turn, features, weights)
        total = parts[0]
        for j in (1, 2, 3):
            total = total + to_sum_ring(parts[j], j).astype(f32)
        own = jnp.square(jnp.maximum(total, 0.0)).astype(bf16)
        return [own] + [from_sum_ring(own, j) for j in (1, 2, 3)]

    hidden_near = activated([up_own] + up_near)
    hidden_far = activated([up_far])
    begun = down_products(turn, [hidden_near], [down_own] + down_near, [], False)
    parts = down_products(turn, [hidden_far], [down_far], begun, True)
    total = parts[0]
    for j, part in zip(others, parts[1:]):
        total = total + to_gather_ring(part, j).astype(f32)
    mine, theirs = total[:few], from_other_core(total[few:])
    mixed_out = residual_scale * normed.astype(f32) + (mine + theirs)
    mean, inverse = scales(group_sums(mixed_out), width)
    out = ((mixed_out - mean) * inverse * gain_out + bias_out).astype(bf16)
    result = jnp.zeros(carried.shape, bf16)
    for d in range(4):
        block = from_plane(out, d) if d else out
        result = lax.dynamic_update_slice(result, block, ((y + d) % 4 * few, 0))
    return result


def solution(mesh):
    in_specs = (
        P("dp", "ra"),
        P("dp", "ra"),
        P("ra"),
        P("ra"),
        P("ra", "cb"),
        P("cb", "ra"),
        P("ra"),
        P("ra"),
    )
    return jax.shard_map(
        layer, mesh=mesh, in_specs=in_specs, out_specs=P("dp", "ra"), check_vma=False
    )
```

```python
import jax
import jax.numpy as jnp
from jax import lax
from jax.experimental import pallas as pl
from jax.experimental.pallas import tpu as pltpu
from jax.sharding import PartitionSpec as P


residual_scale = 2.0**0.25
norm_eps = 1e-05
others = (1, 3, 2)
f32, bf16 = jnp.float32, jnp.bfloat16


def ring_pairs(gathers, distance):
    pairs = []
    for z in range(4):
        for x in range(4):
            for c in range(2):
                if (c == 0) == gathers:
                    source = (z * 4 + (x + distance) % 4) * 2 + c
                else:
                    source = (((z + distance) % 4) * 4 + x) * 2 + c
                pairs.append((source, (z * 4 + x) * 2 + c))
    return pairs


def from_gather_ring(array, distance):
    return lax.ppermute(array, ("ra", "dp"), ring_pairs(True, distance))


def to_gather_ring(array, distance):
    return lax.ppermute(array, ("ra", "dp"), ring_pairs(True, -distance))


def from_sum_ring(array, distance):
    return lax.ppermute(array, ("ra", "dp"), ring_pairs(False, distance))


def to_sum_ring(array, distance):
    return lax.ppermute(array, ("ra", "dp"), ring_pairs(False, -distance))


def from_plane(array, distance):
    return lax.ppermute(array, "cb", [((y + distance) % 4, y) for y in range(4)])


def from_other_core(array):
    return lax.ppermute(array, "dp", [(0, 1), (1, 0)])


def dot(a, b):
    return lax.dot_general(a, b, (((1,), (0,)), ((), ())), preferred_element_type=f32)


def call(body, out_shape, flops, turn, *operands, mib=24):
    size = sum(o.size * o.dtype.itemsize for o in operands)
    specs = [pl.BlockSpec(memory_space=pltpu.SMEM)] if turn is not None else []
    whole = pl.BlockSpec(memory_space=pltpu.VMEM)
    return pl.pallas_call(
        body,
        out_shape=out_shape,
        in_specs=specs + [whole] * len(operands),
        out_specs=[whole] * len(out_shape),
        compiler_params=pltpu.CompilerParams(vmem_limit_bytes=mib * 2**20),
        cost_estimate=pl.CostEstimate(flops=flops, bytes_accessed=size, transcendentals=0),
    )(*([turn] if turn is not None else []), *operands)


def stacked(*blocks):
    def stack(*refs):
        at = 0
        for ref in refs[:-1]:
            refs[-1][at : at + ref.shape[0], :] = ref[...]
            at += ref.shape[0]

    rows = sum(block.shape[0] for block in blocks)
    shape = jax.ShapeDtypeStruct((rows, blocks[0].shape[1]), blocks[0].dtype)
    return call(stack, [shape], 10**8, None, *blocks, mib=9)[0]


def up_products(turn, features, weights):
    rows = features.shape[0] // 4
    flat = [w for ws in weights for w in ws]
    wide = flat[0].shape[1]

    def up(turn_ref, a_ref, *refs):
        w_refs, outs = refs[: len(flat)], refs[len(flat) :]
        for i, out in enumerate(outs):
            start = pl.multiple_of((turn_ref[0] + i) % 4 * rows, rows)
            at = 0
            for n, ws in enumerate(weights):
                total, done = None, 0
                for w_ref in w_refs[at : at + len(ws)]:
                    k = w_ref.shape[0]
                    term = dot(a_ref[pl.ds(start, rows), done : done + k], w_ref[...])
                    total = term if total is None else total + term
                    done += k
                at += len(ws)
                out[:, n * wide : (n + 1) * wide] = total.astype(out.dtype)

    full = wide * len(weights)
    shapes = [jax.ShapeDtypeStruct((rows, full), bf16 if i else f32) for i in range(4)]
    return call(up, shapes, 2 * features.size * full, turn, features, *flat)


def placed(y, blocks):
    rows = blocks[0].shape[0]

    def place(y_ref, *refs):
        for d, ref in enumerate(refs[:-1]):
            start = pl.multiple_of((y_ref[0] + d) % 4 * rows, rows)
            refs[-1][pl.ds(start, rows), :] = ref[...]

    shape = jax.ShapeDtypeStruct((4 * rows, blocks[0].shape[1]), blocks[0].dtype)
    return call(place, [shape], 10**8, y.reshape(1).astype(jnp.int32), *blocks, mib=6)[0]


def down_products(turn, hidden, weights, begun, last):
    rows = hidden[0][0].shape[0]
    chunks = [h for hs in hidden for h in hs]
    flat = [w for ws in weights for w in ws]
    wide = sum(w.shape[0] for w in weights[0]) // 4
    each = flat[0].shape[1]

    def down(turn_ref, *refs):
        h_refs, refs = refs[: len(chunks)], refs[len(chunks) :]
        w_refs, refs = refs[: len(flat)], refs[len(flat) :]
        s_refs, outs = refs[: len(begun)], refs[len(begun) :]
        for i in range(4):
            start = pl.multiple_of((turn_ref[0] + i) % 4 * rows, rows)
            for j, out in enumerate(outs):
                total = s_refs[j][pl.ds(start, rows), :] if begun else None
                at = which = 0
                for n in range(len(hidden)):
                    h_ref = h_refs[4 * n + i]
                    for k in range(h_ref.shape[1] // wide):
                        depth = 0
                        for w_ref in w_refs[at : at + len(weights[which])]:
                            if depth <= j * wide < depth + w_ref.shape[0]:
                                first = j * wide - depth
                                term = dot(
                                    h_ref[:, k * wide : (k + 1) * wide],
                                    w_ref[first : first + wide, :],
                                )
                                total = term if total is None else total + term
                            depth += w_ref.shape[0]
                        at += len(weights[which])
                        which += 1
                out[pl.ds(start, rows), :] = total.astype(out.dtype)

    shapes = [
        jax.ShapeDtypeStruct((4 * rows, each), bf16 if last and j else f32) for j in range(4)
    ]
    flops = 2 * 4 * rows * wide * len(weights) * 4 * each
    return call(down, shapes, flops, turn, *chunks, *flat, *begun)


def own_sums(mixed):
    sums = jnp.stack([jnp.sum(mixed, axis=1), jnp.sum(mixed * mixed, axis=1)])
    return sums.reshape(-1, 128)


def scales(sums, width):
    sums = sums.reshape(2, -1)
    mean = sums[0] / width
    return mean[:, None], lax.rsqrt(sums[1] / width - mean * mean + norm_eps)[:, None]


def group_sums(mixed):
    sums = own_sums(mixed)
    members = lax.axis_size("ra")
    sent = jnp.broadcast_to(sums[None], (members, *sums.shape))
    sums = lax.all_to_all(sent, "ra", 0, 0, tiled=True)
    return sums.sum(axis=0)


def layer(carried, branch_in, gain_in, bias_in, up_weight, down_weight, gain_out, bias_out):
    width = carried.shape[1] * lax.axis_size("ra")
    r, y, c = lax.axis_index("ra"), lax.axis_index("cb"), lax.axis_index("dp")
    z, x = r // 4, r % 4
    a, b = jnp.where(c == 0, x, z), jnp.where(c == 0, z, x)
    turn = ((b - 2 * c) % 4).reshape(1).astype(jnp.int32)
    carried, turn = lax.optimization_barrier((carried, turn))
    held = carried.shape[1]
    few = carried.shape[0] // 4
    wide = up_weight.shape[1] // 8

    def columns_for(distance):
        return (c * 4 + (a + distance) % 4) * wide

    def up_for(distance):
        return lax.dynamic_slice(up_weight, (0, columns_for(distance)), (held, wide))

    def down_for(distance):
        return lax.dynamic_slice(down_weight, (columns_for(distance), 0), (wide, held))

    def gathered(block_for):
        own = block_for(0)
        own_by_y = {d: from_plane(own, d) for d in (1, 3)}
        blocks = [from_gather_ring(block_for(-j), j) for j in others]
        rest = stacked(*blocks)
        rest_by_y = {d: from_plane(rest, d) for d in (1, 3)}
        cut = own.shape[0]
        first = stacked(own_by_y[1], rest_by_y[1][:cut])
        far = (from_plane(first, 1), from_plane(rest_by_y[3][cut:], 3))
        return (own, rest), [(own_by_y[d], rest_by_y[d]) for d in (1, 3)], far

    up_own, up_near, up_far = gathered(up_for)
    down_own, down_near, down_far = gathered(down_for)

    def quarter(array):
        return lax.dynamic_slice(array, (y * few, 0), (few, held)).astype(f32)

    mixed_in = residual_scale * quarter(carried) + quarter(branch_in)
    sums = own_sums(mixed_in)
    sums = sum([from_sum_ring(sums, j) for j in others], sums)
    arrived = [from_gather_ring(sums, j) for j in others]
    sums = sum(arrived, sums)
    mean, inverse = scales(sums, width)
    normed = ((mixed_in - mean) * inverse * gain_in + bias_in).astype(bf16)
    both = stacked(normed, from_other_core(normed))
    features = [both] + [from_gather_ring(both, j) for j in others]
    features = jnp.concatenate(features, axis=1)

    def activated(weights):
        parts = up_products(turn, features, weights)
        total = parts[0]
        for j in (1, 2, 3):
            total = total + to_sum_ring(parts[j], j).astype(f32)
        own = jnp.square(jnp.maximum(total, 0.0)).astype(bf16)
        return [own] + [from_sum_ring(own, j) for j in (1, 2, 3)]

    hidden_near = activated([up_own] + up_near)
    hidden_far = activated([up_far])
    begun = down_products(turn, [hidden_near], [down_own] + down_near, [], False)
    parts = down_products(turn, [hidden_far], [down_far], begun, True)
    total = parts[0]
    for j, part in zip(others, parts[1:]):
        total = total + to_gather_ring(part, j).astype(f32)
    mine, theirs = total[:few], from_other_core(total[few:])
    mixed_out = residual_scale * normed.astype(f32) + (mine + theirs)
    mean, inverse = scales(group_sums(mixed_out), width)
    out = ((mixed_out - mean) * inverse * gain_out + bias_out).astype(bf16)
    return placed(y, [out] + [from_plane(out, d) for d in (1, 2, 3)])


def solution(mesh):
    in_specs = (
        P("dp", "ra"),
        P("dp", "ra"),
        P("ra"),
        P("ra"),
        P("ra", "cb"),
        P("cb", "ra"),
        P("ra"),
        P("ra"),
    )
    return jax.shard_map(
        layer, mesh=mesh, in_specs=in_specs, out_specs=P("dp", "ra"), check_vma=False
    )
```

```python
import jax
import jax.numpy as jnp
from jax import lax
from jax.experimental import pallas as pl
from jax.experimental.pallas import tpu as pltpu
from jax.sharding import PartitionSpec as P


residual_scale = 2.0**0.25
norm_eps = 1e-05
others = (1, 3, 2)
f32, bf16 = jnp.float32, jnp.bfloat16


def ring_pairs(gathers, distance):
    pairs = []
    for z in range(4):
        for x in range(4):
            for c in range(2):
                if (c == 0) == gathers:
                    source = (z * 4 + (x + distance) % 4) * 2 + c
                else:
                    source = (((z + distance) % 4) * 4 + x) * 2 + c
                pairs.append((source, (z * 4 + x) * 2 + c))
    return pairs


def from_gather_ring(array, distance):
    return lax.ppermute(array, ("ra", "dp"), ring_pairs(True, distance))


def to_gather_ring(array, distance):
    return lax.ppermute(array, ("ra", "dp"), ring_pairs(True, -distance))


def from_sum_ring(array, distance):
    return lax.ppermute(array, ("ra", "dp"), ring_pairs(False, distance))


def to_sum_ring(array, distance):
    return lax.ppermute(array, ("ra", "dp"), ring_pairs(False, -distance))


def from_plane(array, distance):
    return lax.ppermute(array, "cb", [((y + distance) % 4, y) for y in range(4)])


def from_other_core(array):
    return lax.ppermute(array, "dp", [(0, 1), (1, 0)])


def dot(a, b):
    return lax.dot_general(a, b, (((1,), (0,)), ((), ())), preferred_element_type=f32)


def call(body, out_shape, flops, turn, *operands, mib=24):
    size = sum(o.size * o.dtype.itemsize for o in operands)
    specs = [pl.BlockSpec(memory_space=pltpu.SMEM)] if turn is not None else []
    whole = pl.BlockSpec(memory_space=pltpu.VMEM)
    return pl.pallas_call(
        body,
        out_shape=out_shape,
        in_specs=specs + [whole] * len(operands),
        out_specs=[whole] * len(out_shape),
        compiler_params=pltpu.CompilerParams(vmem_limit_bytes=mib * 2**20),
        cost_estimate=pl.CostEstimate(flops=flops, bytes_accessed=size, transcendentals=0),
    )(*([turn] if turn is not None else []), *operands)


def stacked(*blocks):
    def stack(*refs):
        at = 0
        for ref in refs[:-1]:
            refs[-1][at : at + ref.shape[0], :] = ref[...]
            at += ref.shape[0]

    rows = sum(block.shape[0] for block in blocks)
    shape = jax.ShapeDtypeStruct((rows, blocks[0].shape[1]), blocks[0].dtype)
    return call(stack, [shape], 10**8, None, *blocks, mib=9)[0]


def up_products(turn, features, weights):
    rows = features.shape[0] // 4
    flat = [w for ws in weights for w in ws]
    wide = flat[0].shape[1]

    def up(turn_ref, a_ref, *refs):
        w_refs, outs = refs[: len(flat)], refs[len(flat) :]
        for i, out in enumerate(outs):
            start = pl.multiple_of((turn_ref[0] + i) % 4 * rows, rows)
            at = 0
            for n, ws in enumerate(weights):
                total, done = None, 0
                for w_ref in w_refs[at : at + len(ws)]:
                    k = w_ref.shape[0]
                    term = dot(a_ref[pl.ds(start, rows), done : done + k], w_ref[...])
                    total = term if total is None else total + term
                    done += k
                at += len(ws)
                out[:, n * wide : (n + 1) * wide] = total.astype(out.dtype)

    full = wide * len(weights)
    shapes = [jax.ShapeDtypeStruct((rows, full), bf16 if i else f32) for i in range(4)]
    return call(up, shapes, 2 * features.size * full, turn, features, *flat)


def placed(y, blocks):
    rows = blocks[0].shape[0]

    def place(y_ref, *refs):
        for d, ref in enumerate(refs[:-1]):
            start = pl.multiple_of((y_ref[0] + d) % 4 * rows, rows)
            refs[-1][pl.ds(start, rows), :] = ref[...]

    shape = jax.ShapeDtypeStruct((4 * rows, blocks[0].shape[1]), blocks[0].dtype)
    return call(place, [shape], 10**8, y.reshape(1).astype(jnp.int32), *blocks, mib=6)[0]


def down_products(turn, hidden, weights, begun, last):
    rows = hidden[0][0].shape[0]
    chunks = [h for hs in hidden for h in hs]
    flat = [w for ws in weights for w in ws]
    wide = sum(w.shape[0] for w in weights[0]) // 4
    each = flat[0].shape[1]

    def down(turn_ref, *refs):
        h_refs, refs = refs[: len(chunks)], refs[len(chunks) :]
        w_refs, refs = refs[: len(flat)], refs[len(flat) :]
        s_refs, outs = refs[: len(begun)], refs[len(begun) :]
        for i in range(4):
            start = pl.multiple_of((turn_ref[0] + i) % 4 * rows, rows)
            for j, out in enumerate(outs):
                total = s_refs[j][pl.ds(start, rows), :] if begun else None
                at = which = 0
                for n in range(len(hidden)):
                    h_ref = h_refs[4 * n + i]
                    for k in range(h_ref.shape[1] // wide):
                        depth = 0
                        for w_ref in w_refs[at : at + len(weights[which])]:
                            if depth <= j * wide < depth + w_ref.shape[0]:
                                first = j * wide - depth
                                term = dot(
                                    h_ref[:, k * wide : (k + 1) * wide],
                                    w_ref[first : first + wide, :],
                                )
                                total = term if total is None else total + term
                            depth += w_ref.shape[0]
                        at += len(weights[which])
                        which += 1
                out[pl.ds(start, rows), :] = total.astype(out.dtype)

    shapes = [
        jax.ShapeDtypeStruct((4 * rows, each), bf16 if last and j else f32) for j in range(4)
    ]
    flops = 2 * 4 * rows * wide * len(weights) * 4 * each
    return call(down, shapes, flops, turn, *chunks, *flat, *begun)


def own_sums(mixed):
    sums = jnp.stack([jnp.sum(mixed, axis=1), jnp.sum(mixed * mixed, axis=1)])
    return sums.reshape(-1, 128)


def scales(sums, width):
    sums = sums.reshape(2, -1)
    mean = sums[0] / width
    return mean[:, None], lax.rsqrt(sums[1] / width - mean * mean + norm_eps)[:, None]


def group_sums(mixed):
    sums = own_sums(mixed)
    members = lax.axis_size("ra")
    sent = jnp.broadcast_to(sums[None], (members, *sums.shape))
    sums = lax.all_to_all(sent, "ra", 0, 0, tiled=True)
    return sums.sum(axis=0)


def layer(carried, branch_in, gain_in, bias_in, up_weight, down_weight, gain_out, bias_out):
    width = carried.shape[1] * lax.axis_size("ra")
    r, y, c = lax.axis_index("ra"), lax.axis_index("cb"), lax.axis_index("dp")
    z, x = r // 4, r % 4
    a, b = jnp.where(c == 0, x, z), jnp.where(c == 0, z, x)
    turn = ((b - 2 * c) % 4).reshape(1).astype(jnp.int32)
    carried, turn = lax.optimization_barrier((carried, turn))
    held = carried.shape[1]
    few = carried.shape[0] // 4
    wide = up_weight.shape[1] // 8

    def columns_for(distance):
        return (c * 4 + (a + distance) % 4) * wide

    def up_for(distance):
        return lax.dynamic_slice(up_weight, (0, columns_for(distance)), (held, wide))

    def down_for(distance):
        return lax.dynamic_slice(down_weight, (columns_for(distance), 0), (wide, held))

    def gathered(block_for):
        own = block_for(0)
        own_by_y = {d: from_plane(own, d) for d in (1, 3)}
        blocks = [from_gather_ring(block_for(-j), j) for j in others]
        rest = stacked(*blocks)
        rest_by_y = {d: from_plane(rest, d) for d in (1, 3)}
        return (own, rest), [(own_by_y[d], rest_by_y[d]) for d in (1, 3)]

    up_own, up_near = gathered(up_for)
    down_own, down_near = gathered(down_for)

    def quarters(array):
        taken = [
            lax.dynamic_slice(array, ((y + d) % 4 * few, 0), (few, held)) for d in (0, 2)
        ]
        return jnp.concatenate(taken, axis=0).astype(f32)

    mixed_in = residual_scale * quarters(carried) + quarters(branch_in)
    sums = own_sums(mixed_in)
    sums = sum([from_sum_ring(sums, j) for j in others], sums)
    arrived = [from_gather_ring(sums, j) for j in others]
    sums = sum(arrived, sums)
    mean, inverse = scales(sums, width)
    normed = ((mixed_in - mean) * inverse * gain_in + bias_in).astype(bf16)
    other = from_other_core(normed)

    def features_of(first):
        both = stacked(normed[first : first + few], other[first : first + few])
        pieces = [both] + [from_gather_ring(both, j) for j in others]
        return jnp.concatenate(pieces, axis=1)

    near_features, far_features = features_of(0), features_of(few)

    def activated(features, weights):
        parts = up_products(turn, features, weights)
        total = parts[0]
        for j in (1, 2, 3):
            total = total + to_sum_ring(parts[j], j).astype(f32)
        own = jnp.square(jnp.maximum(total, 0.0)).astype(bf16)
        return [own] + [from_sum_ring(own, j) for j in (1, 2, 3)]

    def summed(parts):
        total = parts[0]
        for j, part in zip(others, parts[1:]):
            total = total + to_gather_ring(part, j).astype(f32)
        return total

    hidden_near = activated(near_features, [up_own] + up_near)
    hidden_far = activated(far_features, [up_own])
    far_parts = down_products(turn, [hidden_far], [down_own], [], True)
    for_far = summed(far_parts)
    near_parts = down_products(turn, [hidden_near], [down_own] + down_near, [], True)
    total = summed(near_parts) + from_plane(for_far, 2)
    mine, theirs = total[:few], from_other_core(total[few:])
    mixed_out = residual_scale * normed[:few].astype(f32) + (mine + theirs)
    mean, inverse = scales(group_sums(mixed_out), width)
    out = ((mixed_out - mean) * inverse * gain_out + bias_out).astype(bf16)
    return placed(y, [out] + [from_plane(out, d) for d in (1, 2, 3)])


def solution(mesh):
    in_specs = (
        P("dp", "ra"),
        P("dp", "ra"),
        P("ra"),
        P("ra"),
        P("ra", "cb"),
        P("cb", "ra"),
        P("ra"),
        P("ra"),
    )
    return jax.shard_map(
        layer, mesh=mesh, in_specs=in_specs, out_specs=P("dp", "ra"), check_vma=False
    )
```
